32 devices in a mesh: grp: 2 (over y), sp: 4 (over z), tp: 4 (over x, core).
Axes of the slice: x: 2, y: 2, z: 4, core: 2. Of those that a mesh axis runs over, the one named last changes fastest.
Arguments:
- residual_in: bfloat16 [2048, 2048], P(('grp', 'sp', 'tp')), parts along dimension 0, may hold values from -6 to 6
- q_small: bfloat16 [2048, 1024], P(('grp', 'sp'), 'tp'), parts along dimension 0, may hold values from -5 to 5
- k_small: bfloat16 [2048, 256], P(('grp', 'sp'), 'tp'), parts along dimension 0, may hold values from -5 to 5
- v_small: bfloat16 [2048, 256], P(('grp', 'sp'), 'tp'), parts along dimension 0, may hold values from -6 to 6
- q_large: bfloat16 [2048, 1024], P(('grp', 'sp'), 'tp'), parts along dimension 0, may hold values from -5 to 5
- k_large: bfloat16 [2048, 512], P(('grp', 'sp'), 'tp'), parts along dimension 0, may hold values from -5 to 5
- v_large: bfloat16 [2048, 512], P(('grp', 'sp'), 'tp'), parts along dimension 0, may hold values from -6 to 6
- gain_qs: float32 [64], replicated, may hold values from 0.24 to 7.4
- gain_ks: float32 [64], replicated, may hold values from 0.24 to 7.4
- gain_ql: float32 [128], replicated, may hold values from 0.24 to 7.4
- gain_kl: float32 [128], replicated, may hold values from 0.24 to 7.4
- w_out_small: bfloat16 [1024, 2048], P('tp'), may hold values from -0.125 to 0.125
- w_out_large: bfloat16 [1024, 2048], P('tp'), may hold values from -0.125 to 0.125
- g_ffn: float32 [2048], replicated, may hold values from 0.1 to 1.9
- routes: int32 [2048, 4], P(('grp', 'sp', 'tp')), parts along dimension 0, may hold values from 0 to 7, all different within a row; in each aligned block of 64 rows (0 to 63, 64 to 127, ...) at most 64 rows name the same one
- route_w: float32 [2048, 4], P(('grp', 'sp', 'tp')), parts along dimension 0, may hold values from 0.2 to 1
- w_gate: bfloat16 [8, 2048, 1024], P('sp', None, 'tp'), may hold values from -0.125 to 0.125
- w_up: bfloat16 [8, 2048, 1024], P('sp', None, 'tp'), may hold values from -0.125 to 0.125
- w_down: bfloat16 [8, 1024, 2048], P('sp', 'tp'), may hold values from -0.1875 to 0.1875
- ws_gate: bfloat16 [2048, 1024], P(None, 'tp'), may hold values from -0.125 to 0.125
- ws_up: bfloat16 [2048, 1024], P(None, 'tp'), may hold values from -0.125 to 0.125
- ws_down: bfloat16 [1024, 2048], P('tp'), may hold values from -0.1875 to 0.1875
Outputs:
- result: bfloat16 [2048, 2048], P(('grp', 'sp', 'tp')), parts along dimension 0
The draws below stay inside these ranges and needn't reach their ends.
There are 2 independent parts, one for each index of `grp`. The reference program is written for one: setup_inputs(seed, part) draws one part's arguments, and reference() takes and returns one part's arrays. A program takes and returns all parts, laid end to end along the dimension named above; an argument that names none is the same for every part. Nothing has to cross between parts.
Inputs may be any that keep to these rules, and one draw needn't show every extreme that they name: `routes`: each row names 4 different experts. Among the rows of one device no expert is named more than 64 times, a bound that some block reaches.
All inputs are finite; a program needn't handle non-finite values.
Results may differ from the reference program's by a relative error of at most 0.018.
The reference program's roundings to bfloat16 on the way count: a program that leaves them out, or rounds other values in their place, can miss the bound.
Values may be sent and summed in bfloat16 or wider, within the bound.
No kernel may reach another device: no remote copies, remote signals or barrier semaphores. Data moves between devices by JAX's collectives and lax.ppermute only.
A program may use at most 128 MiB of HBM per device.

```python
import math
import jax
import jax.numpy as jnp
import numpy as np
from jax import lax

D = 2048
QA = 16
HS_SMALL = 64
KVA = 4
QB = 8
HS_LARGE = 128
KVB = 4
FF = 1024
FF_SH = 1024
GRID_W = 64
TOPK = 4
TOKENS = 1024
ROWS_DEV = 64
EXPERTS = 8
CAP = 64
N_SP = 4
N_TP = 4


def paired_heads(key, kv_heads, head_width, query_heads):
    key_rows = jax.random.normal(jax.random.fold_in(key, 701 + head_width), (TOKENS, kv_heads, head_width), jnp.float32)
    queries = jax.random.normal(jax.random.fold_in(key, 702 + head_width), (TOKENS, kv_heads, query_heads // kv_heads, head_width), jnp.float32)
    queries = jnp.clip(queries, -5.0, 5.0)
    key_rows = jnp.clip(key_rows, -5.0, 5.0)
    return (queries.reshape(TOKENS, query_heads * head_width), key_rows.reshape(TOKENS, kv_heads * head_width))


def positive_gain(key, channels, salt):
    return jnp.exp(jax.random.uniform(jax.random.fold_in(key, salt), (channels,), jnp.float32, -1.4, 1.4))


def draw_q_small(key, part):
    return paired_heads(key, KVA, HS_SMALL, QA)[0].astype(jnp.bfloat16)


def draw_k_small(key, part):
    return paired_heads(key, KVA, HS_SMALL, QA)[1].astype(jnp.bfloat16)


def draw_q_large(key, part):
    return paired_heads(key, KVB, HS_LARGE, QB)[0].astype(jnp.bfloat16)


def draw_k_large(key, part):
    return paired_heads(key, KVB, HS_LARGE, QB)[1].astype(jnp.bfloat16)


def draw_gain_qs(key, part):
    return positive_gain(key, HS_SMALL, 811)


def draw_gain_ks(key, part):
    return positive_gain(key, HS_SMALL, 812)


def draw_gain_ql(key, part):
    return positive_gain(key, HS_LARGE, 813)


def draw_gain_kl(key, part):
    return positive_gain(key, HS_LARGE, 814)


def levels(key, shape, shards, low, top_value):
    loudness, own = 1.0, jax.random.fold_in(key, 6)
    for dim, shards_of in shards:
        heights = jnp.exp(jax.random.uniform(jax.random.fold_in(own, dim), (shards_of,), jnp.float32, low / len(shards), top_value / len(shards)))
        loudness = loudness * jnp.repeat(heights, shape[dim] // shards_of).reshape([-1 if axis == dim else 1 for axis in range(len(shape))])
    return loudness


def deal_out(key, own, number, rows, amount, top, bound, skew):
    sequence = jax.random.permutation(key, amount)
    heavy_load, usual = load_shares(amount, rows * top, bound, skew, True), load_shares(amount, rows * top, bound, skew, False)
    places = jnp.arange(amount)

    def named(tallies, turn):
        used = int((tallies > 0).sum())
        fixed = max(1, used // 4)
        moved = fixed + (places - fixed + turn * (used - fixed)) % max(1, amount - fixed)
        return jnp.zeros((amount,), jnp.int32).at[sequence[jnp.where(places < fixed, places, moved)]].set(jnp.asarray(tallies, jnp.int32))

    tallies = jnp.where(number % 4 == 0, named(heavy_load, number // 4), named(usual, number - number // 4 - 1))
    mixed = jax.random.permutation(jax.random.fold_in(own, 3), amount)
    giver, taker = mixed[0:amount // 2 * 2:2], mixed[1:amount // 2 * 2:2]
    margin = jnp.minimum(tallies[giver] - 1, bound - tallies[taker]) // 2
    margin = jnp.where((giver == sequence[0]) | (taker == sequence[0]) | (tallies[taker] == 0), 0, jnp.maximum(margin, 0))
    moved = jax.random.randint(jax.random.fold_in(own, 4), (amount // 2,), 0, 1 << 20) % (margin + 1)
    tallies = tallies.at[giver].add(-moved).at[taker].add(moved)
    items = jnp.searchsorted(jnp.cumsum(tallies), jnp.arange(rows * top), side="right").astype(jnp.int32)
    table = items.reshape(top, rows).T
    table = table[jax.random.permutation(jax.random.fold_in(own, 1), rows)]
    turn = jax.random.randint(jax.random.fold_in(own, 2), (rows, 1), 0, top)
    return jnp.take_along_axis(table, (jnp.arange(top)[None, :] + turn) % top, axis=1)


def load_shares(number_of, total, limit, skew, full):
    loads = [(1 << 20) // math.isqrt(rank ** skew) + 1 for rank in range(1, number_of + 1)]
    largest = limit if full else min(limit, max(-(-total // number_of), total * loads[0] // sum(loads)))
    least = 1 if total - largest >= number_of - 1 else 0
    holding, rest = [largest] + [least] * (number_of - 1), total - largest - least * (number_of - 1)
    while rest > 0:
        candidates = [i for i in range(1, number_of) if holding[i] < largest] or [i for i in range(1, number_of) if holding[i] < limit]
        pool, budget = sum([loads[i] for i in candidates]), rest
        for i in candidates:
            addition = min(limit - holding[i], max(1, budget * loads[i] // pool), rest)
            holding[i] = holding[i] + addition
            rest = rest - addition
    return np.array(holding)


def scatter_about(stream_key, shape, spread, bound, cuts=(), kind=jnp.bfloat16):
    level = levels(stream_key, shape, cuts, -0.22, 0.18) if cuts else 1.0
    entries = jax.random.normal(stream_key, shape, jnp.float32) * spread * level
    return jnp.minimum(jnp.maximum(entries, -bound), bound).astype(kind)


def setup_inputs(seed: int = 0, part: int = 0) -> dict:
    splits = jax.random.split(jax.random.key(seed), 23)
    part_keys = jax.random.split(jax.random.fold_in(splits[22], part), 23)
    residual_in = scatter_about(part_keys[0], (TOKENS, D), 1.0, 6.0, ((0, 16),))
    q_small = draw_q_small(jax.random.fold_in(jax.random.fold_in(splits[22], part), 71), part)
    k_small = draw_k_small(jax.random.fold_in(jax.random.fold_in(splits[22], part), 71), part)
    v_small = scatter_about(part_keys[3], (TOKENS, KVA * HS_SMALL), 1.0, 6.0, ((0, 4), (1, 4)))
    q_large = draw_q_large(jax.random.fold_in(jax.random.fold_in(splits[22], part), 71), part)
    k_large = draw_k_large(jax.random.fold_in(jax.random.fold_in(splits[22], part), 71), part)
    v_large = scatter_about(part_keys[6], (TOKENS, KVB * HS_LARGE), 1.0, 6.0, ((0, 4), (1, 4)))
    gain_qs = draw_gain_qs(jax.random.fold_in(splits[22], 71), part)
    gain_ks = draw_gain_ks(jax.random.fold_in(splits[22], 71), part)
    gain_ql = draw_gain_ql(jax.random.fold_in(splits[22], 71), part)
    gain_kl = draw_gain_kl(jax.random.fold_in(splits[22], 71), part)
    w_out_small = scatter_about(splits[11], (QA * HS_SMALL, D), (QA * HS_SMALL + QB * HS_LARGE) ** -0.5, 0.125, ((0, 4),))
    w_out_large = scatter_about(splits[12], (QB * HS_LARGE, D), (QA * HS_SMALL + QB * HS_LARGE) ** -0.5, 0.125, ((0, 4),))
    g_ffn = jnp.clip(1.0 + 0.18 * jax.random.normal(splits[13], (D,), jnp.float32), 0.1, 1.9)
    routes_keys = jax.random.split(jax.random.fold_in(part_keys[14], 1), TOKENS // ROWS_DEV)
    routes_turns = jax.random.permutation(jax.random.fold_in(part_keys[14], 3), TOKENS // ROWS_DEV)
    routes = jax.vmap(lambda own, number: deal_out(jax.random.fold_in(part_keys[14], 2), own, number, ROWS_DEV, EXPERTS, TOPK, CAP, 2))(routes_keys, routes_turns).reshape((TOKENS, TOPK))
    route_w = jnp.clip(0.2 + 0.8 * jax.random.uniform(part_keys[15], (TOKENS, TOPK), jnp.float32) ** levels(part_keys[15], (TOKENS, TOPK), ((0, 16),), -0.2, 0.2), 0.2, 1.0)
    w_gate = scatter_about(splits[16], (EXPERTS, D, FF), D ** -0.5, 0.125, ((0, 4), (2, 4)))
    w_up = scatter_about(splits[17], (EXPERTS, D, FF), D ** -0.5, 0.125, ((0, 4), (2, 4)))
    w_down = scatter_about(splits[18], (EXPERTS, FF, D), FF ** -0.5, 0.1875, ((0, 4), (1, 4)))
    ws_gate = scatter_about(splits[19], (D, FF_SH), D ** -0.5, 0.125, ((1, 4),))
    ws_up = scatter_about(splits[20], (D, FF_SH), D ** -0.5, 0.125, ((1, 4),))
    ws_down = scatter_about(splits[21], (FF_SH, D), FF_SH ** -0.5, 0.1875, ((0, 4),))
    return {"residual_in": residual_in, "q_small": q_small, "k_small": k_small, "v_small": v_small, "q_large": q_large, "k_large": k_large, "v_large": v_large, "gain_qs": gain_qs, "gain_ks": gain_ks, "gain_ql": gain_ql, "gain_kl": gain_kl, "w_out_small": w_out_small, "w_out_large": w_out_large, "g_ffn": g_ffn, "routes": routes, "route_w": route_w, "w_gate": w_gate, "w_up": w_up, "w_down": w_down, "ws_gate": ws_gate, "ws_up": ws_up, "ws_down": ws_down}


norm_eps = 1e-06
rope_base = 10000.0

def rounded(values):
    return lax.optimization_barrier(values.astype(jnp.bfloat16)).astype(jnp.float32)

def rotate_pairs(values, angles):
    front_half, back_half = jnp.split(values, 2, axis=-1)
    cosine_vals = jnp.cos(angles)[:, None, :]
    sine_vals = jnp.sin(angles)[:, None, :]
    return jnp.concatenate([front_half * cosine_vals - back_half * sine_vals, front_half * sine_vals + back_half * cosine_vals], axis=-1)

def norm_rotate(heads_in, gain, positions, grid_width):
    channels = gain.shape[0]
    values = heads_in.astype(jnp.float32).reshape(heads_in.shape[0], -1, channels)
    values = values * lax.rsqrt(lax.optimization_barrier(jnp.mean(values * values, axis=-1, keepdims=True)) + norm_eps) * gain
    quarter = channels // 4
    inverse = 1.0 / rope_base ** (jnp.arange(quarter, dtype=jnp.float32) / quarter)
    grid_rows = (positions // grid_width).astype(jnp.float32)
    grid_cols = (positions % grid_width).astype(jnp.float32)
    half_width = channels // 2
    turned = jnp.concatenate([rotate_pairs(values[..., :half_width], grid_rows[:, None] * inverse[None, :]), rotate_pairs(values[..., half_width:], grid_cols[:, None] * inverse[None, :])], axis=-1)
    return turned.astype(jnp.bfloat16)

def attend(queries, key_rows, value_rows):
    tokens, heads, channels = queries.shape
    kv_heads = key_rows.shape[1]
    group = heads // kv_heads
    block_rows = math.gcd(tokens, 256)
    blocks = queries.reshape(tokens // block_rows, block_rows, kv_heads, group, channels)
    keys32 = key_rows.astype(jnp.float32)
    values32 = value_rows.astype(jnp.float32)

    def one_block(query_block):
        scores = jnp.einsum('qkgd,skd->kgqs', query_block.astype(jnp.float32), keys32) * channels ** (-0.5)
        peak_val = lax.optimization_barrier(jnp.max(scores, axis=-1, keepdims=True))
        weights_raw = jnp.exp(scores - peak_val)
        totals = lax.optimization_barrier(jnp.sum(weights_raw, axis=-1))
        weights = rounded(weights_raw)
        mixture = jnp.einsum('kgqs,skd->qkgd', weights, values32)
        mixture = mixture / jnp.transpose(totals, (2, 0, 1))[..., None]
        return mixture.astype(jnp.bfloat16)
    result = lax.map(one_block, blocks)
    return result.reshape(tokens, heads * channels)

def split_down(hidden, down_w, pieces):
    columns = hidden.shape[1] // pieces
    summed = jnp.zeros((hidden.shape[0], down_w.shape[1]), jnp.float32)
    for device in range(pieces):
        term = jnp.dot(hidden[:, device * columns:(device + 1) * columns], down_w[device * columns:(device + 1) * columns], preferred_element_type=jnp.float32)
        summed = summed + rounded(term)
    return summed

def reference(residual_in, q_small, k_small, v_small, q_large, k_large, v_large, gain_qs, gain_ks, gain_ql, gain_kl, w_out_small, w_out_large, g_ffn, routes, route_w, w_gate, w_up, w_down, ws_gate, ws_up, ws_down):
    positions = jnp.arange(TOKENS, dtype=jnp.int32)
    heads_small = attend(norm_rotate(q_small, gain_qs, positions, GRID_W), norm_rotate(k_small, gain_ks, positions, GRID_W), v_small.reshape(TOKENS, KVA, HS_SMALL))
    heads_large = attend(norm_rotate(q_large, gain_ql, positions, GRID_W), norm_rotate(k_large, gain_kl, positions, GRID_W), v_large.reshape(TOKENS, KVB, HS_LARGE))
    small_cols = QA * HS_SMALL // N_TP
    large_cols = QB * HS_LARGE // N_TP
    head_sum = jnp.zeros((TOKENS, D), jnp.float32)
    for device in range(N_TP):
        term = jnp.dot(heads_small[:, device * small_cols:(device + 1) * small_cols], w_out_small[device * small_cols:(device + 1) * small_cols], preferred_element_type=jnp.float32)
        term = term + jnp.dot(heads_large[:, device * large_cols:(device + 1) * large_cols], w_out_large[device * large_cols:(device + 1) * large_cols], preferred_element_type=jnp.float32)
        head_sum = head_sum + rounded(term)
    stream32 = rounded(residual_in.astype(jnp.float32) + head_sum)
    normed = (stream32 * lax.rsqrt(lax.optimization_barrier(jnp.mean(stream32 * stream32, axis=-1, keepdims=True)) + norm_eps) * g_ffn).astype(jnp.bfloat16)
    assigned = TOKENS * TOPK
    flat_ids = routes.reshape(assigned)
    flat_weights = jnp.concatenate([route_w.reshape(assigned), jnp.zeros((1,), jnp.float32)])
    padded_rows = jnp.concatenate([normed, jnp.zeros((1, D), jnp.bfloat16)], axis=0)
    most_rows = N_SP * N_TP * CAP

    def one_expert(routed, inputs):
        expert, gate_w, up_w, down_w = inputs
        picked = jnp.nonzero(flat_ids == expert, size=most_rows, fill_value=assigned)[0].astype(jnp.int32)
        owners = jnp.where(picked < assigned, picked // TOPK, TOKENS).astype(jnp.int32)
        rows_in = padded_rows[owners]
        gate_act = jnp.dot(rows_in, gate_w, preferred_element_type=jnp.float32)
        up_act = jnp.dot(rows_in, up_w, preferred_element_type=jnp.float32)
        hidden = (jax.nn.silu(gate_act) * up_act).astype(jnp.bfloat16)
        expert_out = split_down(hidden, down_w, N_TP).astype(jnp.bfloat16)
        routed = routed.at[owners].add(flat_weights[picked][:, None] * expert_out.astype(jnp.float32))
        return (routed, None)
    routed, _ = lax.scan(one_expert, jnp.zeros((TOKENS + 1, D), jnp.float32), (jnp.arange(EXPERTS, dtype=jnp.int32), w_gate, w_up, w_down))
    shared_hidden = (jax.nn.silu(jnp.dot(normed, ws_gate, preferred_element_type=jnp.float32)) * jnp.dot(normed, ws_up, preferred_element_type=jnp.float32)).astype(jnp.bfloat16)
    shared = split_down(shared_hidden, ws_down, N_TP)
    return (stream32 + routed[:TOKENS] + shared).astype(jnp.bfloat16)
```

```python
import math

import jax
import jax.numpy as jnp
from jax import lax
from jax.sharding import PartitionSpec as P

GRID_W = 64
TOPK = 4


norm_eps = 1e-06
rope_base = 10000.0
far_below = -1e30


def rotate_pairs(values, angles):
    front_half, back_half = jnp.split(values, 2, axis=-1)
    cosine_vals = jnp.cos(angles)[:, None, :]
    sine_vals = jnp.sin(angles)[:, None, :]
    return jnp.concatenate(
        [
            front_half * cosine_vals - back_half * sine_vals,
            front_half * sine_vals + back_half * cosine_vals,
        ],
        axis=-1,
    )


def norm_rotate(heads_in, gain, positions, grid_width):
    channels = gain.shape[0]
    values = heads_in.astype(jnp.float32).reshape(heads_in.shape[0], -1, channels)
    values = values * lax.rsqrt(jnp.mean(values * values, axis=-1, keepdims=True) + norm_eps) * gain
    quarter = channels // 4
    inverse = 1.0 / rope_base ** (jnp.arange(quarter, dtype=jnp.float32) / quarter)
    grid_rows = (positions // grid_width).astype(jnp.float32)
    grid_cols = (positions % grid_width).astype(jnp.float32)
    half_width = channels // 2
    turned = jnp.concatenate(
        [
            rotate_pairs(values[..., :half_width], grid_rows[:, None] * inverse[None, :]),
            rotate_pairs(values[..., half_width:], grid_cols[:, None] * inverse[None, :]),
        ],
        axis=-1,
    )
    return turned.astype(jnp.bfloat16)


def absorb(carried, segment, queries):
    peak_val, totals, mixture = carried
    kv_heads = queries.shape[1]
    channels = queries.shape[3]
    pairs = segment.reshape(segment.shape[0], 2, kv_heads, channels)
    scores = jnp.einsum(
        "qkgd,skd->kgqs", queries, pairs[:, 0], preferred_element_type=jnp.float32
    ) * channels ** (-0.5)
    new_peak = jnp.maximum(peak_val, jnp.max(scores, axis=-1))
    weights_raw = jnp.exp(scores - new_peak[..., None])
    shrink = jnp.exp(peak_val - new_peak)
    totals = totals * shrink + jnp.sum(weights_raw, axis=-1)
    update = jnp.einsum(
        "kgqs,skd->qkgd",
        weights_raw.astype(jnp.bfloat16),
        pairs[:, 1],
        preferred_element_type=jnp.float32,
    )
    mixture = mixture * jnp.transpose(shrink, (2, 0, 1))[..., None] + update
    return (new_peak, totals, mixture)


def absorb_blocks(carried, segment, queries):
    row_count = segment.shape[0]
    block_rows = math.gcd(row_count, 1024)
    stacked = segment.reshape(row_count // block_rows, block_rows, segment.shape[1])

    def fold_step(inner, key_block):
        return (absorb(inner, key_block, queries), None)

    carried, _ = lax.scan(fold_step, carried, stacked)
    return carried


def start_state(queries):
    local_rows, kv_heads, group, channels = queries.shape
    return (
        jnp.full((kv_heads, group, local_rows), far_below, jnp.float32),
        jnp.zeros((kv_heads, group, local_rows), jnp.float32),
        jnp.zeros(queries.shape, jnp.float32),
    )


def finish(carried):
    peak_val, totals, mixture = carried
    heads_out = mixture / jnp.transpose(totals, (2, 0, 1))[..., None]
    return heads_out.reshape(heads_out.shape[0], -1).astype(jnp.bfloat16)


def local_routed(
    residual_in,
    q_small,
    k_small,
    v_small,
    q_large,
    k_large,
    v_large,
    gain_qs,
    gain_ks,
    gain_ql,
    gain_kl,
    w_out_small,
    w_out_large,
    g_ffn,
    routes,
    route_w,
    w_gate,
    w_up,
    w_down,
    ws_gate,
    ws_up,
    ws_down,
):
    local_rows = q_small.shape[0]
    positions = lax.axis_index("sp") * local_rows + jnp.arange(local_rows, dtype=jnp.int32)
    query_small = norm_rotate(q_small, gain_qs, positions, GRID_W)
    key_small = norm_rotate(k_small, gain_ks, positions, GRID_W)
    query_large = norm_rotate(q_large, gain_ql, positions, GRID_W)
    key_large = norm_rotate(k_large, gain_kl, positions, GRID_W)
    query_small = query_small.reshape(local_rows, key_small.shape[1], -1, gain_qs.shape[0])
    query_large = query_large.reshape(local_rows, key_large.shape[1], -1, gain_ql.shape[0])
    pack_small = jnp.concatenate([key_small.reshape(local_rows, -1), v_small], axis=1)
    pack_large = jnp.concatenate([key_large.reshape(local_rows, -1), v_large], axis=1)
    segment = (
        lax.all_gather(pack_small, "sp", axis=0, tiled=True),
        lax.all_gather(pack_large, "sp", axis=0, tiled=True),
    )
    heads_small = finish(absorb_blocks(start_state(query_small), segment[0], query_small))
    heads_large = finish(absorb_blocks(start_state(query_large), segment[1], query_large))
    tp_count = lax.axis_size("tp")
    sp_count = lax.axis_size("sp")
    rows_dev = local_rows // tp_count
    head_sum = lax.psum_scatter(
        (
            jnp.dot(heads_small, w_out_small, preferred_element_type=jnp.float32)
            + jnp.dot(heads_large, w_out_large, preferred_element_type=jnp.float32)
        ).astype(jnp.bfloat16),
        "tp",
        scatter_dimension=0,
        tiled=True,
    ).astype(jnp.float32)
    stream = (residual_in.astype(jnp.float32) + head_sum).astype(jnp.bfloat16)
    stream32 = lax.optimization_barrier(stream).astype(jnp.float32)
    normed = (
        stream32
        * lax.rsqrt(jnp.mean(stream32 * stream32, axis=-1, keepdims=True) + norm_eps)
        * g_ffn
    ).astype(jnp.bfloat16)
    channels = normed.shape[1]
    segment = lax.all_gather(normed, "tp", axis=0, tiled=True)
    gate_act = jnp.dot(segment, ws_gate, preferred_element_type=jnp.float32)
    up_act = jnp.dot(segment, ws_up, preferred_element_type=jnp.float32)
    hidden_shared = (jax.nn.silu(gate_act) * up_act).astype(jnp.bfloat16)
    shared = lax.psum_scatter(
        jnp.dot(hidden_shared, ws_down, preferred_element_type=jnp.float32).astype(jnp.bfloat16),
        "tp",
        scatter_dimension=0,
        tiled=True,
    ).astype(jnp.float32)
    local_experts = w_gate.shape[0]
    experts = local_experts * sp_count
    capacity = max(2, 2 * rows_dev * TOPK // experts)
    flat_ids = routes.reshape(-1)
    one_hot = (flat_ids[:, None] == jnp.arange(experts, dtype=jnp.int32)[None, :]).astype(jnp.int32)
    slot_ids = jnp.sum((jnp.cumsum(one_hot, axis=0) - 1) * one_hot, axis=1)
    targets = flat_ids * capacity + slot_ids
    owners = jnp.arange(rows_dev * TOPK, dtype=jnp.int32) // TOPK
    outbox = jnp.zeros((experts * capacity, channels), jnp.bfloat16).at[targets].set(normed[owners])
    arrived = lax.all_to_all(outbox, "sp", split_axis=0, concat_axis=0, tiled=True)
    arrived = lax.all_gather(
        arrived.reshape(sp_count, 1, local_experts, capacity, channels), "tp", axis=1, tiled=True
    )
    gate_act = jnp.einsum("abecd,edf->abecf", arrived, w_gate, preferred_element_type=jnp.float32)
    up_act = jnp.einsum("abecd,edf->abecf", arrived, w_up, preferred_element_type=jnp.float32)
    hidden = (jax.nn.silu(gate_act) * up_act).astype(jnp.bfloat16)
    partial_value = jnp.einsum(
        "abecf,efd->abecd", hidden, w_down, preferred_element_type=jnp.float32
    )
    summed = lax.psum_scatter(
        partial_value.astype(jnp.bfloat16), "tp", scatter_dimension=1, tiled=True
    )
    returned = lax.all_to_all(
        summed.reshape(sp_count * local_experts * capacity, channels),
        "sp",
        split_axis=0,
        concat_axis=0,
        tiled=True,
    )
    picked = returned[targets].reshape(rows_dev, TOPK, channels).astype(jnp.float32)
    routed = jnp.sum(picked * route_w[..., None], axis=1)
    return (stream32 + routed + shared).astype(jnp.bfloat16)


def flip_pairs(count, bit):
    return [(i, i ^ bit) for i in range(count)]


def ring_pairs(count):
    return [(i, (i + 1) % count) for i in range(count)]


def swap_core(values, tp_count):
    return lax.ppermute(values, "tp", flip_pairs(tp_count, 1))


def swap_chip(values, tp_count):
    return lax.ppermute(values, "tp", flip_pairs(tp_count, 2))


def pass_on(values, sp_count):
    return lax.ppermute(values, "sp", ring_pairs(sp_count))


def add_rounded(first, second):
    return (first.astype(jnp.float32) + second.astype(jnp.float32)).astype(jnp.bfloat16)


def relative_rows(values, me, rows_dev):
    blocks = values.reshape(-1, rows_dev, values.shape[1])
    picked = [lax.dynamic_index_in_dim(blocks, me ^ flip, 0, keepdims=False) for flip in (0, 2, 1, 3)]
    return jnp.concatenate(picked, axis=0)


def reduce_rows(partial, tp_count):
    half = partial.shape[0] // 2
    mine = add_rounded(partial[:half], swap_core(partial[half:], tp_count))
    quarter = half // 2
    return mine[:quarter].astype(jnp.float32) + swap_chip(mine[quarter:], tp_count).astype(jnp.float32)


def local_dense(
    residual_in,
    q_small,
    k_small,
    v_small,
    q_large,
    k_large,
    v_large,
    gain_qs,
    gain_ks,
    gain_ql,
    gain_kl,
    w_out_small,
    w_out_large,
    g_ffn,
    routes,
    route_w,
    w_gate,
    w_up,
    w_down,
    ws_gate,
    ws_up,
    ws_down,
):
    tp_count = lax.axis_size("tp")
    sp_count = lax.axis_size("sp")
    me = lax.axis_index("tp")
    layer = lax.axis_index("sp")
    local_rows = q_small.shape[0]
    rows_dev = local_rows // tp_count
    positions = layer * local_rows + jnp.arange(local_rows, dtype=jnp.int32)
    key_small = norm_rotate(k_small, gain_ks, positions, GRID_W)
    key_large = norm_rotate(k_large, gain_kl, positions, GRID_W)
    pack = jnp.concatenate(
        [key_small.reshape(local_rows, -1), v_small, key_large.reshape(local_rows, -1), v_large], axis=1
    )
    segment = lax.all_gather(pack, "sp", axis=0, tiled=True)
    split = 2 * k_small.shape[1]

    local_experts = w_gate.shape[0]
    experts = local_experts * sp_count
    expert_ids = jnp.arange(experts, dtype=jnp.int32)
    token_w = jnp.sum(
        jnp.where(routes[None] == expert_ids[:, None, None], route_w[None], 0.0), axis=2
    )
    token_w = jnp.concatenate([token_w, swap_chip(token_w, tp_count)], axis=1)
    token_w = jnp.concatenate([token_w, swap_core(token_w, tp_count)], axis=1)
    weights = [token_w]
    for _ in range(sp_count - 1):
        weights.append(pass_on(weights[-1], sp_count))
    weights = [
        lax.dynamic_slice_in_dim(w, layer * local_experts, local_experts, axis=0).T for w in weights
    ]

    turned = relative_rows(positions[:, None], me, rows_dev)[:, 0]
    query_small = norm_rotate(relative_rows(q_small, me, rows_dev), gain_qs, turned, GRID_W)
    query_large = norm_rotate(relative_rows(q_large, me, rows_dev), gain_ql, turned, GRID_W)
    query_small = query_small.reshape(local_rows, key_small.shape[1], -1, gain_qs.shape[0])
    query_large = query_large.reshape(local_rows, key_large.shape[1], -1, gain_ql.shape[0])
    heads_small = finish(absorb(start_state(query_small), segment[:, :split], query_small))
    heads_large = finish(absorb(start_state(query_large), segment[:, split:], query_large))
    partial = (
        jnp.dot(heads_small, w_out_small, preferred_element_type=jnp.float32)
        + jnp.dot(heads_large, w_out_large, preferred_element_type=jnp.float32)
    ).astype(jnp.bfloat16)
    head_sum = reduce_rows(partial, tp_count)
    stream = (residual_in.astype(jnp.float32) + head_sum).astype(jnp.bfloat16)
    stream32 = lax.optimization_barrier(stream).astype(jnp.float32)
    normed = (
        stream32
        * lax.rsqrt(jnp.mean(stream32 * stream32, axis=-1, keepdims=True) + norm_eps)
        * g_ffn
    ).astype(jnp.bfloat16)

    def gated(rows, gate_w, up_w):
        gate_act = jnp.dot(rows, gate_w, preferred_element_type=jnp.float32)
        up_act = jnp.dot(rows, up_w, preferred_element_type=jnp.float32)
        return (jax.nn.silu(gate_act) * up_act).astype(jnp.bfloat16)

    own = [normed]
    for _ in range(sp_count - 1):
        own.append(pass_on(own[-1], sp_count))
    across = [swap_chip(rows, tp_count) for rows in own]
    sums = [None] * sp_count
    for step in [*range(1, sp_count), 0]:
        mine = jnp.concatenate([own[step], across[step]], axis=0)
        rows = jnp.concatenate([mine, swap_core(mine, tp_count)], axis=0)
        total = 0.0
        for e in range(local_experts):
            hidden = gated(rows, w_gate[e], w_up[e])
            total = total + weights[step][:, e : e + 1] * jnp.dot(
                hidden, w_down[e], preferred_element_type=jnp.float32
            )
        if step == 0:
            hidden = gated(rows, ws_gate, ws_up)
            total = total + jnp.dot(hidden, ws_down, preferred_element_type=jnp.float32)
        sums[step] = reduce_rows(total.astype(jnp.bfloat16), tp_count)
    moving = sums[1] if sp_count > 1 else None
    for step in [*range(2, sp_count), 0][: sp_count - 1]:
        moving = sums[step] + pass_on(moving.astype(jnp.bfloat16), sp_count).astype(jnp.float32)
    if moving is None:
        moving = sums[0]
    return (stream32 + moving).astype(jnp.bfloat16)


def local(*args):
    q_small, routes, w_gate = args[1], args[14], args[16]
    tp_count = lax.axis_size("tp")
    experts = w_gate.shape[0] * lax.axis_size("sp")
    rows_dev = q_small.shape[0] // tp_count
    capacity = max(2, 2 * rows_dev * routes.shape[1] // experts)
    if capacity >= rows_dev and tp_count == 4:
        return local_dense(*args)
    return local_routed(*args)


def solution(mesh):
    placed = (
        P(("grp", "sp", "tp"), None),
        P(("grp", "sp"), "tp"),
        P(("grp", "sp"), "tp"),
        P(("grp", "sp"), "tp"),
        P(("grp", "sp"), "tp"),
        P(("grp", "sp"), "tp"),
        P(("grp", "sp"), "tp"),
        P(),
        P(),
        P(),
        P(),
        P("tp", None),
        P("tp", None),
        P(),
        P(("grp", "sp", "tp"), None),
        P(("grp", "sp", "tp"), None),
        P("sp", None, "tp"),
        P("sp", None, "tp"),
        P("sp", "tp", None),
        P(None, "tp"),
        P(None, "tp"),
        P("tp", None),
    )
    return jax.shard_map(
        local, mesh=mesh, in_specs=placed, out_specs=P(("grp", "sp", "tp"), None), check_vma=False
    )
```
